32 devices in a mesh: sp: 16 (over z, y, x), tp: 2 (over core).
Axes of the slice: x: 2, y: 2, z: 4, core: 2. Of those that a mesh axis runs over, the one named last changes fastest.
Arguments:
- glu_value: bfloat16 [4096, 1024], P('sp', 'tp'), may hold values from -12 to 12
- glu_gate: bfloat16 [4096, 1024], P('sp', 'tp'), may hold values from -8 to 8
- conv_kernel: bfloat16 [31, 1024], P(None, 'tp'), may hold values from -1 to 1
- conv_bias: float32 [1024], P('tp'), may hold values from -1.5 to 1.5
- group_gain: float32 [1024], P('tp'), may hold values from 0.1 to 1.9
- group_shift: float32 [1024], P('tp'), may hold values from -2.5 to 2.5
- out_weight: bfloat16 [1024, 2048], replicated, may hold values from -0.1875 to 0.1875
- residual: bfloat16 [4096, 2048], P(('sp', 'tp')), may hold values from -12 to 12
- ffn_gain: float32 [2048], replicated, may hold values from 0.1 to 1.9
- expert_pick: int32 [4096, 2], P(('sp', 'tp')), may hold values from 0 to 31, as said below
- pair_logits: float32 [4096, 2], P(('sp', 'tp')), may hold values from -1.2 to 1.2
- group_prob: float32 [4096], P(('sp', 'tp')), may hold values from 0.5 to 1
- gate_weight: bfloat16 [32, 2048, 512], P(('sp', 'tp')), may hold values from -0.125 to 0.125
- up_weight: bfloat16 [32, 2048, 512], P(('sp', 'tp')), may hold values from -0.125 to 0.125
- down_weight: bfloat16 [32, 512, 2048], P(('sp', 'tp')), may hold values from -0.75 to 0.75
Outputs:
- result: bfloat16 [4096, 2048], P(('sp', 'tp'))
The draws below stay inside these ranges and needn't reach their ends.
Inputs may be any that keep to these rules, and one draw needn't show every extreme that they name: `expert_pick`: both picks of a token are different experts of the same group of 8 consecutive experts. Among the 128 tokens of one device (aligned blocks of rows) no expert is picked more than 16 times, and in every such block some expert is picked exactly 16 times.
All inputs are finite; a program needn't handle non-finite values.
Results may differ from the reference program's by a relative error of at most 0.014.
Values may be sent and summed in bfloat16 or wider, within the bound.
A program may use at most 64 MiB of HBM per device.

```python
import math
import jax
import jax.numpy as jnp
from jax import lax

D = 2048
CONV = 1024
CONV_GROUPS = 8
KERNEL = 31
FFE = 512
GROUPS = 4
TOK_DEV = 128
TOKENS = 4096
EXPERTS = 32
CAP = 16
N_SP = 16
N_TP = 2


def scaled_normal(key, row_total, columns, lowest, highest):
    subkeys = jax.random.split(key, 3)
    normal_part = jax.random.normal(subkeys[0], (row_total, columns), jnp.float32)
    row_scale = jnp.exp(jax.random.uniform(subkeys[1], (row_total, 1), jnp.float32, jnp.log(lowest), jnp.log(highest)))
    column_scale = jnp.exp(jax.random.uniform(subkeys[2], (1, columns), jnp.float32, jnp.log(lowest), jnp.log(highest)))
    return normal_part * row_scale * column_scale


def draw_residual(key, part):
    scaled = scaled_normal(key, TOKENS, D, 0.2, 2.0)
    return jnp.clip(scaled, -12.0, 12.0).astype(jnp.bfloat16)


def draw_glu_value(key, part):
    scaled = scaled_normal(key, TOKENS, CONV, 0.3, 3.0)
    return jnp.clip(scaled, -12.0, 12.0).astype(jnp.bfloat16)


def draw_expert_pick(key, part):
    per_group = EXPERTS // GROUPS
    pairs = per_group * CAP // 2
    universe = GROUPS * pairs
    blocks = TOKENS // TOK_DEV
    subkeys = jax.random.split(key, 3)
    full_group = jax.random.randint(subkeys[0], (), 0, GROUPS)

    def label_order(label_key):
        return jax.random.permutation(label_key, per_group)
    labels = jax.vmap(label_order)(jax.random.split(subkeys[1], GROUPS)).astype(jnp.int32)
    slot_index = jnp.arange(universe, dtype=jnp.int32)
    slot_group = slot_index // pairs
    slot_pair = slot_index % pairs
    forced = (slot_group == full_group) & (slot_pair < CAP)

    def one_block(block_key):
        inner = jax.random.split(block_key, 3)
        scores = jax.random.randint(inner[0], (universe,), 0, 1 << 18) * universe + slot_index
        scores = jnp.where(forced, slot_pair - CAP, scores)
        chosen = jnp.argsort(scores, stable=True)[:TOK_DEV]
        chosen = chosen[jax.random.permutation(inner[1], TOK_DEV)]
        group_of = slot_group[chosen]
        low_label = slot_pair[chosen] // CAP
        high_label = low_label + per_group // 2
        first_expert = group_of * per_group + labels[group_of, low_label]
        second_expert = group_of * per_group + labels[group_of, high_label]
        flipped = jax.random.randint(inner[2], (TOK_DEV,), 0, 2)
        left_pick = jnp.where(flipped == 1, second_expert, first_expert)
        right_pick = jnp.where(flipped == 1, first_expert, second_expert)
        return jnp.stack([left_pick, right_pick], axis=1)
    picked = jax.vmap(one_block)(jax.random.split(subkeys[2], blocks))
    return picked.reshape(TOKENS, 2).astype(jnp.int32)


def block_scale(key, shape, cuts, low, top_value):
    gain = 1.0
    for position, parts in cuts:
        draws = jax.random.uniform(jax.random.fold_in(jax.random.fold_in(key, 6), position), (parts,), jnp.float32, low / len(cuts), top_value / len(cuts))
        gain = gain * jnp.repeat(jnp.exp(draws), shape[position] // parts).reshape((-1,) + (1,) * (len(shape) - 1 - position))
    return gain


def scatter_about(rng, shape, spread, limit, pieces=(), kind=jnp.bfloat16):
    level = block_scale(rng, shape, pieces, -0.22, 0.18) if pieces else 1.0
    values = jax.random.normal(rng, shape, jnp.float32) * spread * level
    return jnp.minimum(jnp.maximum(values, -limit), limit).astype(kind)


def setup_inputs(seed: int = 0) -> dict:
    key_of = jax.random.split(jax.random.key(seed), 16)
    glu_value = draw_glu_value(jax.random.fold_in(key_of[15], 71), 0)
    glu_gate = scatter_about(key_of[1], (TOKENS, CONV), 1.5, 8.0, ((0, 16), (1, 2)))
    conv_kernel = scatter_about(key_of[2], (KERNEL, CONV), KERNEL ** -0.5, 1.0, ((1, 2),))
    conv_bias = scatter_about(key_of[3], (CONV,), 0.3, 1.5, ((0, 2),), jnp.float32)
    group_gain = jnp.clip(1.0 + 0.18 * jax.random.normal(key_of[4], (CONV,), jnp.float32), 0.1, 1.9)
    group_shift = scatter_about(key_of[5], (CONV,), 0.5, 2.5, ((0, 2),), jnp.float32)
    out_weight = scatter_about(key_of[6], (CONV, D), CONV ** -0.5, 0.1875)
    residual = draw_residual(jax.random.fold_in(key_of[15], 71), 0)
    ffn_gain = jnp.clip(1.0 + 0.18 * jax.random.normal(key_of[8], (D,), jnp.float32), 0.1, 1.9)
    expert_pick = draw_expert_pick(jax.random.fold_in(key_of[15], 71), 0)
    pair_logits = scatter_about(key_of[10], (TOKENS, 2), 0.3, 1.2, ((0, 32),), jnp.float32)
    group_prob = jnp.clip(jnp.exp(math.log(1.0) - 0.6931472 * jax.random.uniform(key_of[11], (TOKENS,), jnp.float32) ** block_scale(key_of[11], (TOKENS,), ((0, 32),), -0.2, 0.2)), 0.5, 1.0)
    gate_weight = scatter_about(key_of[12], (EXPERTS, D, FFE), D ** -0.5, 0.125, ((0, 32),))
    up_weight = scatter_about(key_of[13], (EXPERTS, D, FFE), D ** -0.5, 0.125, ((0, 32),))
    down_weight = scatter_about(key_of[14], (EXPERTS, FFE, D), (FFE // 8) ** -0.5, 0.75, ((0, 32),))
    return dict(glu_value=glu_value, glu_gate=glu_gate, conv_kernel=conv_kernel, conv_bias=conv_bias, group_gain=group_gain, group_shift=group_shift, out_weight=out_weight, residual=residual, ffn_gain=ffn_gain, expert_pick=expert_pick, pair_logits=pair_logits, group_prob=group_prob, gate_weight=gate_weight, up_weight=up_weight, down_weight=down_weight)


EPS = 1e-06

def conv_module(glu_value, glu_gate, conv_kernel, conv_bias, group_gain, group_shift):
    glued_rows = (glu_value.astype(jnp.float32) * jax.nn.sigmoid(glu_gate.astype(jnp.float32))).astype(jnp.bfloat16)
    reach_rows = conv_kernel.shape[0] - 1
    length = glued_rows.shape[0]
    padded = jnp.pad(glued_rows, ((reach_rows, 0), (0, 0))).astype(jnp.float32)
    kernel = conv_kernel.astype(jnp.float32)
    summed = jnp.zeros(glued_rows.shape, jnp.float32) + conv_bias.astype(jnp.float32)
    for offset in range(reach_rows + 1):
        summed = summed + kernel[offset] * padded[offset:offset + length]
    grouped = summed.reshape(length, CONV_GROUPS, -1)
    centre = lax.optimization_barrier(jnp.mean(grouped, axis=-1, keepdims=True))
    variance = lax.optimization_barrier(jnp.mean(jnp.square(grouped - centre), axis=-1, keepdims=True))
    leveled = ((grouped - centre) * lax.rsqrt(variance + EPS)).reshape(length, -1)
    return jax.nn.silu(leveled * group_gain + group_shift).astype(jnp.bfloat16)

def experts_apply(normed, expert_pick, gate_weight, up_weight, down_weight):
    picks = expert_pick.shape[1]
    slot_experts = expert_pick.reshape(-1)
    slot_total = slot_experts.shape[0]
    most_rows = N_SP * N_TP * CAP
    onehot = (slot_experts[:, None] == jnp.arange(EXPERTS, dtype=jnp.int32)[None, :]).astype(jnp.int32)
    before = (jnp.cumsum(onehot, axis=0) - onehot).astype(jnp.int32)
    slot_rank = lax.optimization_barrier(jnp.sum(before * onehot, axis=1)).astype(jnp.int32)
    slot_place = (slot_experts * most_rows + slot_rank).astype(jnp.int32)
    source_flat = jnp.full((EXPERTS * most_rows,), slot_total, jnp.int32)
    source_flat = source_flat.at[slot_place].set(jnp.arange(slot_total, dtype=jnp.int32))
    source_table = source_flat.reshape(EXPERTS, most_rows)
    padded_rows = jnp.concatenate([normed, jnp.zeros((1, normed.shape[1]), normed.dtype)], axis=0)

    def apply_expert(inputs):
        source_index, gate_part, up_part, down_part = inputs
        picked = padded_rows[source_index // picks]
        gate_out = jnp.dot(picked, gate_part, preferred_element_type=jnp.float32)
        up_out = jnp.dot(picked, up_part, preferred_element_type=jnp.float32)
        active = (jax.nn.silu(gate_out) * up_out).astype(jnp.bfloat16)
        return jnp.dot(active, down_part, preferred_element_type=jnp.float32).astype(jnp.bfloat16)
    answers = lax.map(apply_expert, (source_table, gate_weight, up_weight, down_weight))
    flat_answers = answers.reshape(EXPERTS * most_rows, -1)
    return flat_answers[slot_place].reshape(-1, picks, normed.shape[1])

def reference(glu_value, glu_gate, conv_kernel, conv_bias, group_gain, group_shift, out_weight, residual, ffn_gain, expert_pick, pair_logits, group_prob, gate_weight, up_weight, down_weight):
    mixed_rows = conv_module(glu_value, glu_gate, conv_kernel, conv_bias, group_gain, group_shift)
    projected = jnp.dot(mixed_rows, out_weight, preferred_element_type=jnp.float32)
    hidden = (residual.astype(jnp.float32) + projected).astype(jnp.bfloat16)
    hidden_full = hidden.astype(jnp.float32)
    scale_rows = lax.rsqrt(lax.optimization_barrier(jnp.mean(hidden_full * hidden_full, axis=-1, keepdims=True)) + EPS)
    normed = (hidden_full * scale_rows * ffn_gain).astype(jnp.bfloat16)
    answer = experts_apply(normed, expert_pick, gate_weight, up_weight, down_weight)
    first_share = group_prob * jax.nn.sigmoid(pair_logits[:, 0] - pair_logits[:, 1])
    second_share = group_prob * jax.nn.sigmoid(pair_logits[:, 1] - pair_logits[:, 0])
    combined = hidden_full + first_share[:, None] * answer[:, 0].astype(jnp.float32)
    combined = combined + second_share[:, None] * answer[:, 1].astype(jnp.float32)
    return combined.astype(jnp.bfloat16)
```

```python
import functools

import jax
import jax.numpy as jnp
from jax import lax
from jax.experimental import pallas as pl
from jax.experimental.pallas import tpu as pltpu
from jax.sharding import PartitionSpec as P

CONV_GROUPS = 8


EPS = 1e-06


def from_behind(value, axis, by):
    peers = lax.axis_size(axis)
    pairs = [(i, i + by) for i in range(peers) if 0 <= i + by < peers]
    return lax.ppermute(value, axis, pairs)

PLANES = 4
MESH = pl.DeviceIdType.MESH
ORDER = (1, 3, 2)
ROWS_MIN = 16


def moe_kernel(
    cap,
    slot,
    normed_ref,
    hidden_ref,
    place_ref,
    meta_ref,
    gate_hbm,
    up_hbm,
    down_hbm,
    out_ref,
    zsend,
    zrecv,
    mrecv,
    xsend,
    xrecv,
    asend,
    arecv,
    csend,
    cret,
    gate_v,
    up_v,
    down_v,
    wsem,
    zss,
    zrs,
    mss,
    mrs,
    xss,
    xrs,
    ass,
    ars,
    css,
    crs,
):
    n_tp = lax.axis_size("tp")
    chips = lax.axis_size("sp") // PLANES
    peers = chips * n_tp
    sp = lax.axis_index("sp")
    tp = lax.axis_index("tp")
    z = sp // chips
    here = sp % chips
    j = here * n_tp + tp
    slots = peers * slot
    group_rows = zsend.shape[1]

    def plane(d):
        if d == 1:
            return z + 1 - 2 * (z % 2)
        if d == 2:
            return z + 2 - 4 * (z // 2)
        return PLANES - 1 - z

    def mate(d):
        return (plane(d) * chips + here, tp)

    def peer(k):
        return (z * chips + k // n_tp, k % n_tp)

    def zcopy(d):
        return pltpu.make_async_remote_copy(
            src_ref=zsend.at[d], dst_ref=zrecv.at[d], send_sem=zss.at[d], recv_sem=zrs.at[d],
            device_id=mate(d), device_id_type=MESH,
        )

    def mcopy(d):
        return pltpu.make_async_remote_copy(
            src_ref=meta_ref.at[d], dst_ref=mrecv.at[d], send_sem=mss.at[d], recv_sem=mrs.at[d],
            device_id=mate(d), device_id_type=MESH,
        )

    def ccopy(d):
        return pltpu.make_async_remote_copy(
            src_ref=csend.at[d], dst_ref=cret.at[d], send_sem=css.at[d], recv_sem=crs.at[d],
            device_id=mate(d), device_id_type=MESH,
        )

    def xcopy(d, o):
        rows = pl.ds(o * slot, slot)
        return pltpu.make_async_remote_copy(
            src_ref=xsend.at[d, rows], dst_ref=xrecv.at[d, rows],
            send_sem=xss.at[d, o], recv_sem=xrs.at[d, o],
            device_id=peer((j + o) % peers), device_id_type=MESH,
        )

    def acopy(d, o):
        rows = pl.ds(o * slot, slot)
        return pltpu.make_async_remote_copy(
            src_ref=asend.at[d, rows], dst_ref=arecv.at[d, rows],
            send_sem=ass.at[d, o], recv_sem=ars.at[d, o],
            device_id=peer((j + peers - o) % peers), device_id_type=MESH,
        )

    weights = [
        pltpu.make_async_copy(gate_hbm.at[0], gate_v, wsem.at[0]),
        pltpu.make_async_copy(up_hbm.at[0], up_v, wsem.at[1]),
        pltpu.make_async_copy(down_hbm.at[0], down_v, wsem.at[2]),
    ]
    for copy in weights:
        copy.start()

    barrier = pltpu.get_barrier_semaphore()
    for d in ORDER:
        pl.semaphore_signal(barrier, inc=1, device_id=mate(d), device_id_type=MESH)
    for o in range(1, peers):
        pl.semaphore_signal(
            barrier, inc=1, device_id=peer((j + o) % peers), device_id_type=MESH
        )
    for d in (0,) + ORDER:
        picked = jnp.dot(
            place_ref[d * group_rows : (d + 1) * group_rows, :],
            normed_ref[...],
            preferred_element_type=jnp.float32,
        )
        zsend[d] = picked.astype(jnp.bfloat16)
    pl.semaphore_wait(barrier, len(ORDER) + peers - 1)
    for d in ORDER:
        mcopy(d).start()
    for d in ORDER:
        zcopy(d).start()

    def places(d):
        meta = meta_ref[0] if d == 0 else mrecv[d]
        row = lax.broadcasted_iota(jnp.int32, (slots, group_rows), 0).astype(jnp.float32)
        shift = (j * slot).astype(jnp.float32)
        out = []
        for k in range(2):
            at = meta[k : k + 1, :group_rows] - shift
            at = jnp.where(at < 0, at + slots, at)
            out.append(row == at)
        shares = [meta[2 + k : 3 + k, :group_rows] for k in range(2)]
        return out, shares

    def entry(d):
        if d:
            mcopy(d).wait_recv()
            zcopy(d).wait_recv()
        at, _ = places(d)
        chosen = jnp.where(at[0] | at[1], 1.0, 0.0).astype(jnp.bfloat16)
        rows = zsend[0] if d == 0 else zrecv[d]
        spread = jnp.dot(chosen, rows, preferred_element_type=jnp.float32).astype(jnp.bfloat16)
        xrecv[d, :slot] = spread[:slot]
        xsend[d, slot:] = spread[slot:]
        for o in range(1, peers):
            xcopy(d, o).start()

    def expert(d):
        for o in range(1, peers):
            xcopy(d, o).wait_recv()
        rows = xrecv[d]
        gate_out = jnp.dot(rows, gate_v[...], preferred_element_type=jnp.float32)
        up_out = jnp.dot(rows, up_v[...], preferred_element_type=jnp.float32)
        active = (gate_out / (1.0 + jnp.exp(-gate_out)) * up_out).astype(jnp.bfloat16)
        answer = jnp.dot(active, down_v[...], preferred_element_type=jnp.float32)
        answer = answer.astype(jnp.bfloat16)
        arecv[d, :slot] = answer[:slot]
        asend[d, slot:] = answer[slot:]
        for o in range(1, peers):
            acopy(d, o).start()

    def combine(d):
        for o in range(1, peers):
            acopy(d, o).wait_recv()
        at, shares = places(d)
        mix = jnp.where(at[0], shares[0], 0.0) + jnp.where(at[1], shares[1], 0.0)
        high = mix.astype(jnp.bfloat16)
        low = (mix - high.astype(jnp.float32)).astype(jnp.bfloat16)
        dims = (((0,), (0,)), ((), ()))
        answers = arecv[d]
        total = lax.dot_general(high, answers, dims, preferred_element_type=jnp.float32)
        total += lax.dot_general(low, answers, dims, preferred_element_type=jnp.float32)
        if d == 0:
            cret[0] = total.astype(jnp.bfloat16)
        else:
            csend[d] = total.astype(jnp.bfloat16)
            ccopy(d).start()

    a, b, c = ORDER
    entry(0)
    entry(a)
    for copy in weights:
        copy.wait()
    expert(0)
    entry(b)
    expert(a)
    combine(0)
    entry(c)
    combine(a)
    expert(b)
    combine(b)
    expert(c)
    combine(c)

    for d in ORDER:
        ccopy(d).wait_recv()
    dims = (((0,), (0,)), ((), ()))
    gathered = cret[...].reshape(PLANES * group_rows, cret.shape[2])
    total = lax.dot_general(place_ref[...], gathered, dims, preferred_element_type=jnp.float32)
    out_ref[...] = (hidden_ref[...].astype(jnp.float32) + total).astype(jnp.bfloat16)

    for d in ORDER:
        mcopy(d).wait_send()
        zcopy(d).wait_send()
        ccopy(d).wait_send()
    for d in range(PLANES):
        for o in range(1, peers):
            xcopy(d, o).wait_send()
            acopy(d, o).wait_send()


def moe(normed, hidden, place, meta, gate_weight, up_weight, down_weight, cap):
    rows, width = normed.shape
    peers = lax.axis_size("sp") // PLANES * lax.axis_size("tp")
    group_rows = place.shape[0] // PLANES
    slot = max(cap, ROWS_MIN)
    slots = peers * slot
    bf16 = jnp.bfloat16
    vmem = pl.BlockSpec(memory_space=pltpu.VMEM)
    hbm = pl.BlockSpec(memory_space=pl.ANY)
    dma = pltpu.SemaphoreType.DMA
    return pl.pallas_call(
        functools.partial(moe_kernel, cap, slot),
        out_shape=jax.ShapeDtypeStruct((rows, width), bf16),
        in_specs=[vmem] * 4 + [hbm] * 3,
        out_specs=vmem,
        scratch_shapes=[
            pltpu.VMEM((PLANES, group_rows, width), bf16),
            pltpu.VMEM((PLANES, group_rows, width), bf16),
            pltpu.VMEM(meta.shape, jnp.float32),
            pltpu.VMEM((PLANES, slots, width), bf16),
            pltpu.VMEM((PLANES, slots, width), bf16),
            pltpu.VMEM((PLANES, slots, width), bf16),
            pltpu.VMEM((PLANES, slots, width), bf16),
            pltpu.VMEM((PLANES, group_rows, width), bf16),
            pltpu.VMEM((PLANES, group_rows, width), bf16),
            pltpu.VMEM(gate_weight.shape[1:], bf16),
            pltpu.VMEM(up_weight.shape[1:], bf16),
            pltpu.VMEM(down_weight.shape[1:], bf16),
            dma((3,)),
            dma((PLANES,)),
            dma((PLANES,)),
            dma((PLANES,)),
            dma((PLANES,)),
            dma((PLANES, peers)),
            dma((PLANES, peers)),
            dma((PLANES, peers)),
            dma((PLANES, peers)),
            dma((PLANES,)),
            dma((PLANES,)),
        ],
        compiler_params=pltpu.CompilerParams(
            collective_id=0, has_side_effects=True, vmem_limit_bytes=60 * 1024 * 1024
        ),
    )(normed, hidden, place, meta, gate_weight, up_weight, down_weight)


def routing(expert_pick, pair_logits, group_prob, cap):
    tokens = expert_pick.shape[0]
    chips = lax.axis_size("sp") // PLANES
    peers = chips * lax.axis_size("tp")
    group_rows = peers * cap // 2
    z = lax.axis_index("sp") // chips
    order = jnp.arange(tokens, dtype=jnp.int32)
    earlier = order[:, None] < order[None, :]
    picks = [expert_pick[:, 0], expert_pick[:, 1]]
    ranks = []
    for pick in picks:
        same = (picks[0][:, None] == pick[None, :]) | (picks[1][:, None] == pick[None, :])
        ranks.append(jnp.sum((same & earlier).astype(jnp.int32), axis=0))
    group = picks[0] // peers
    row = jnp.sum(((group[:, None] == group[None, :]) & earlier).astype(jnp.int32), axis=0)
    at = (group ^ z) * group_rows + row
    rows = jnp.arange(PLANES * group_rows, dtype=jnp.int32)
    hit = rows[:, None] == at[None, :]
    place = hit.astype(jnp.bfloat16)
    slot = max(cap, ROWS_MIN)
    first = group_prob * jax.nn.sigmoid(pair_logits[:, 0] - pair_logits[:, 1])
    second = group_prob * jax.nn.sigmoid(pair_logits[:, 1] - pair_logits[:, 0])
    fields = [(picks[k] % peers * slot + ranks[k] + 1).astype(jnp.float32) for k in range(2)]
    fields = [jnp.sum(jnp.where(hit, f[None, :], 0.0), axis=1) for f in fields + [first, second]]
    fields = [jnp.where(f > 0, f - 1.0, 65536.0) for f in fields[:2]] + fields[2:]
    meta = jnp.stack(fields).reshape(len(fields), PLANES, group_rows)
    meta = jnp.pad(meta, ((0, 8 - len(fields)), (0, 0), (0, 128 - group_rows)))
    return place, meta.transpose(1, 0, 2)


def local(
    glu_value,
    glu_gate,
    conv_kernel,
    conv_bias,
    group_gain,
    group_shift,
    out_weight,
    residual,
    ffn_gain,
    expert_pick,
    pair_logits,
    group_prob,
    gate_weight,
    up_weight,
    down_weight,
):
    glued_rows = (
        glu_value.astype(jnp.float32) * jax.nn.sigmoid(glu_gate.astype(jnp.float32))
    ).astype(jnp.bfloat16)
    reach_rows = conv_kernel.shape[0] - 1
    length = glued_rows.shape[0]
    earlier = from_behind(glued_rows[length - reach_rows :], "sp", 1)
    extended = jnp.concatenate([earlier, glued_rows], axis=0).astype(jnp.float32)
    kernel = conv_kernel.astype(jnp.float32)
    summed = jnp.zeros(glued_rows.shape, jnp.float32) + conv_bias
    for offset in range(reach_rows + 1):
        summed = summed + kernel[offset] * extended[offset : offset + length]
    groups_here = CONV_GROUPS // lax.axis_size("tp")
    grouped = summed.reshape(length, groups_here, -1)
    centre = jnp.mean(grouped, axis=-1, keepdims=True)
    variance = jnp.mean(jnp.square(grouped - centre), axis=-1, keepdims=True)
    leveled = ((grouped - centre) * lax.rsqrt(variance + EPS)).reshape(length, -1)
    mixed_rows = jax.nn.silu(leveled * group_gain + group_shift).astype(jnp.bfloat16)
    local_rows = residual.shape[0]
    regrouped = lax.all_to_all(mixed_rows, "tp", split_axis=0, concat_axis=1, tiled=True)
    projected = jnp.dot(regrouped, out_weight, preferred_element_type=jnp.float32)
    hidden = (residual.astype(jnp.float32) + projected).astype(jnp.bfloat16)
    hidden_full = hidden.astype(jnp.float32)
    scale_rows = lax.rsqrt(jnp.mean(hidden_full * hidden_full, axis=-1, keepdims=True) + EPS)
    normed = (hidden_full * scale_rows * ffn_gain).astype(jnp.bfloat16)
    experts_all = lax.axis_size("sp") * lax.axis_size("tp")
    capacity = 4 * local_rows // experts_all
    place, meta = routing(expert_pick, pair_logits, group_prob, capacity)
    return moe(normed, hidden, place, meta, gate_weight, up_weight, down_weight, capacity)


def solution(mesh):
    in_specs = (
        P("sp", "tp"),
        P("sp", "tp"),
        P(None, "tp"),
        P("tp"),
        P("tp"),
        P("tp"),
        P(),
        P(("sp", "tp"), None),
        P(),
        P(("sp", "tp"), None),
        P(("sp", "tp"), None),
        P(("sp", "tp")),
        P(("sp", "tp"), None, None),
        P(("sp", "tp"), None, None),
        P(("sp", "tp"), None, None),
    )
    out_specs = P(("sp", "tp"), None)
    return jax.shard_map(local, mesh=mesh, in_specs=in_specs, out_specs=out_specs, check_vma=False)
```

```python
import functools

import jax
import jax.numpy as jnp
from jax import lax
from jax.experimental import pallas as pl
from jax.experimental.pallas import tpu as pltpu
from jax.sharding import PartitionSpec as P

CONV_GROUPS = 8


EPS = 1e-06


PLANES = 4
MESH = pl.DeviceIdType.MESH
ORDER = (1, 3, 2)
ROWS_MIN = 16


def layer_kernel(
    cap,
    slot,
    value_ref,
    gate_ref,
    taps_ref,
    bias_ref,
    gain_ref,
    shift_ref,
    residual_ref,
    ffn_ref,
    pick_ref,
    logit_ref,
    prob_ref,
    out_hbm,
    gate_hbm,
    up_hbm,
    down_hbm,
    out_ref,
    glued,
    hsend,
    hrecv,
    mixed,
    mrest,
    place_ref,
    meta_ref,
    normed_ref,
    hidden_ref,
    proj,
    out_v,
    zsend,
    zrecv,
    mrecv,
    xsend,
    xrecv,
    asend,
    arecv,
    csend,
    cret,
    gate_v,
    up_v,
    down_v,
    wsem,
    hss,
    hrs,
    tss,
    trs,
    zss,
    zrs,
    mss,
    mrs,
    xss,
    xrs,
    ass,
    ars,
    css,
    crs,
):
    n_tp = lax.axis_size("tp")
    chips = lax.axis_size("sp") // PLANES
    peers = chips * n_tp
    sp = lax.axis_index("sp")
    tp = lax.axis_index("tp")
    n_sp = lax.axis_size("sp")
    z = sp // chips
    here = sp % chips
    tokens = residual_ref.shape[0]
    length, channels = value_ref.shape
    reach = taps_ref.shape[0] - 1
    lead = hsend.shape[0]
    j = here * n_tp + tp
    slots = peers * slot
    group_rows = zsend.shape[1]

    def plane(d):
        if d == 1:
            return z + 1 - 2 * (z % 2)
        if d == 2:
            return z + 2 - 4 * (z // 2)
        return PLANES - 1 - z

    def mate(d):
        return (plane(d) * chips + here, tp)

    def peer(k):
        return (z * chips + k // n_tp, k % n_tp)

    def zcopy(d):
        return pltpu.make_async_remote_copy(
            src_ref=zsend.at[d], dst_ref=zrecv.at[d], send_sem=zss.at[d], recv_sem=zrs.at[d],
            device_id=mate(d), device_id_type=MESH,
        )

    def mcopy(d):
        return pltpu.make_async_remote_copy(
            src_ref=meta_ref.at[d], dst_ref=mrecv.at[d], send_sem=mss.at[d], recv_sem=mrs.at[d],
            device_id=mate(d), device_id_type=MESH,
        )

    def ccopy(d):
        return pltpu.make_async_remote_copy(
            src_ref=csend.at[d], dst_ref=cret.at[d], send_sem=css.at[d], recv_sem=crs.at[d],
            device_id=mate(d), device_id_type=MESH,
        )

    def xcopy(d, o):
        rows = pl.ds(o * slot, slot)
        return pltpu.make_async_remote_copy(
            src_ref=xsend.at[d, rows], dst_ref=xrecv.at[d, rows],
            send_sem=xss.at[d, o], recv_sem=xrs.at[d, o],
            device_id=peer((j + o) % peers), device_id_type=MESH,
        )

    def acopy(d, o):
        rows = pl.ds(o * slot, slot)
        return pltpu.make_async_remote_copy(
            src_ref=asend.at[d, rows], dst_ref=arecv.at[d, rows],
            send_sem=ass.at[d, o], recv_sem=ars.at[d, o],
            device_id=peer((j + peers - o) % peers), device_id_type=MESH,
        )

    def halo():
        return pltpu.make_async_remote_copy(
            src_ref=hsend, dst_ref=hrecv, send_sem=hss.at[0], recv_sem=hrs.at[0],
            device_id=((sp + 1) % n_sp, tp), device_id_type=MESH,
        )

    def tcopy(o):
        other = (tp + o) % n_tp
        rows = pl.ds(pl.multiple_of(other * tokens, tokens), tokens)
        return pltpu.make_async_remote_copy(
            src_ref=mixed.at[rows], dst_ref=mrest.at[o], send_sem=tss.at[o], recv_sem=trs.at[o],
            device_id=(sp, other), device_id_type=MESH,
        )

    out_copy = pltpu.make_async_copy(out_hbm, out_v, wsem.at[3])
    out_copy.start()
    weights = [
        pltpu.make_async_copy(gate_hbm.at[0], gate_v, wsem.at[0]),
        pltpu.make_async_copy(up_hbm.at[0], up_v, wsem.at[1]),
        pltpu.make_async_copy(down_hbm.at[0], down_v, wsem.at[2]),
    ]
    for copy in weights:
        copy.start()

    barrier = pltpu.get_barrier_semaphore()
    for d in ORDER:
        pl.semaphore_signal(barrier, inc=1, device_id=mate(d), device_id_type=MESH)
    for o in range(1, peers):
        pl.semaphore_signal(
            barrier, inc=1, device_id=peer((j + o) % peers), device_id_type=MESH
        )
    pl.semaphore_signal(
        barrier, inc=1, device_id=((sp + 1) % n_sp, tp), device_id_type=MESH
    )
    pl.semaphore_signal(
        barrier, inc=1, device_id=((sp + n_sp - 1) % n_sp, tp), device_id_type=MESH
    )

    f32 = jnp.float32
    bf16 = jnp.bfloat16
    block = 64
    for start in range(length - block, -1, -block):
        rows = slice(start, start + block)
        gated = value_ref[rows].astype(f32) / (1.0 + jnp.exp(-gate_ref[rows].astype(f32)))
        gated = gated.astype(bf16)
        glued[lead + start : lead + start + block] = gated.astype(f32)
        if start == length - block:
            hsend[...] = gated[block - lead :]
    pl.semaphore_wait(barrier, len(ORDER) + peers + 1)
    halo().start()

    lane = lax.broadcasted_iota(jnp.int32, (tokens, 128), 1)
    picks = pick_ref[...].astype(f32)
    logits = logit_ref[...]
    cols = [picks[:, 0:1], picks[:, 1:2], logits[:, 0:1], logits[:, 1:2]]
    wide = jnp.zeros((tokens, 128), f32)
    for k in range(4):
        wide = jnp.where(lane == k, cols[k], wide)
    tall = wide.T
    rows_of = [tall[k : k + 1, :] for k in range(4)]
    square = (tokens, tokens)
    earlier = lax.broadcasted_iota(jnp.int32, square, 0) < lax.broadcasted_iota(
        jnp.int32, square, 1
    )

    def group_of(pick):
        total = jnp.zeros(pick.shape, f32)
        for q in range(1, PLANES):
            total += jnp.where(pick >= (q * peers), 1.0, 0.0)
        return total

    def count(hit):
        return jnp.sum(jnp.where(hit & earlier, 1.0, 0.0), axis=0, keepdims=True)

    ranks = [count((cols[0] == r) | (cols[1] == r)) for r in rows_of[:2]]
    group_row = group_of(rows_of[0])
    spot = count(group_of(cols[0]) == group_row)
    away = group_row.astype(jnp.int32) ^ z
    at_row = away.astype(f32) * group_rows + spot
    row_id = lax.broadcasted_iota(jnp.int32, (PLANES * group_rows, tokens), 0).astype(f32)
    place_ref[...] = jnp.where(row_id == at_row, 1.0, 0.0).astype(bf16)
    gap = rows_of[2] - rows_of[3]
    shares = [prob_ref[...] / (1.0 + jnp.exp(-gap)), prob_ref[...] / (1.0 + jnp.exp(gap))]
    fields = [jnp.ones((1, tokens), f32)]
    for k in range(2):
        fields += [rows_of[k] - group_row * peers, ranks[k]]
    for share in shares:
        for _ in range(3):
            part = share.astype(bf16).astype(f32)
            fields.append(part)
            share = share - part
    field_id = lax.broadcasted_iota(jnp.int32, (16, tokens), 0)
    table = jnp.zeros((16, tokens), f32)
    for k, field in enumerate(fields):
        table = jnp.where(field_id == k, field, table)
    table = table.astype(bf16)
    meta_ref[...] = jnp.zeros(meta_ref.shape, f32)
    for d in range(PLANES):
        part = lax.dot_general(
            table,
            place_ref[d * group_rows : (d + 1) * group_rows, :],
            (((1,), (1,)), ((), ())),
            preferred_element_type=f32,
        )
        empty = (1.0 - part[0:1]) * 65536.0
        meta_ref[d, 0:1, :group_rows] = part[1:2] * slot + part[2:3] + empty
        meta_ref[d, 1:2, :group_rows] = part[3:4] * slot + part[4:5] + empty
        meta_ref[d, 2:3, :group_rows] = part[5:6] + part[6:7] + part[7:8]
        meta_ref[d, 3:4, :group_rows] = part[8:9] + part[9:10] + part[10:11]
    for d in ORDER:
        mcopy(d).start()

    wide_group = channels * n_tp // CONV_GROUPS
    taps = taps_ref[...].astype(f32)
    for start in range(length - block, -1, -block):
        if start == 0:
            halo().wait_recv()
            keep = jnp.where(sp > 0, 1.0, 0.0)
            glued[:lead] = hrecv[...].astype(f32) * keep
        for low_lane in range(0, channels, wide_group):
            part = slice(low_lane, low_lane + wide_group)
            total = jnp.zeros((block, wide_group), f32) + bias_ref[:, part]
            for offset in range(reach + 1):
                first = start + lead - reach + offset
                total += taps[offset : offset + 1, part] * glued[first : first + block, part]
            centre = jnp.mean(total, axis=-1, keepdims=True)
            total = total - centre
            variance = jnp.mean(total * total, axis=-1, keepdims=True)
            level = total * lax.rsqrt(variance + EPS)
            level = level * gain_ref[:, part] + shift_ref[:, part]
            mixed[start : start + block, part] = (level / (1.0 + jnp.exp(-level))).astype(bf16)
    for o in range(1, n_tp):
        tcopy(o).start()
    out_copy.wait()

    def weight_rows(which):
        return out_v[pl.ds(pl.multiple_of(which * channels, channels), channels), :]

    own = mixed[pl.ds(pl.multiple_of(tp * tokens, tokens), tokens), :]
    proj[...] = jnp.dot(own, weight_rows(tp), preferred_element_type=f32)
    for o in range(1, n_tp):
        tcopy(o).wait_recv()
        proj[...] += jnp.dot(
            mrest[o], weight_rows((tp + n_tp - o) % n_tp), preferred_element_type=f32
        )
    for start in range(0, tokens, 16):
        rows = slice(start, start + 16)
        hidden = (residual_ref[rows].astype(f32) + proj[rows]).astype(bf16)
        hidden_ref[rows] = hidden
        full = hidden.astype(f32)
        scale = lax.rsqrt(jnp.mean(full * full, axis=-1, keepdims=True) + EPS)
        normed_ref[rows] = (full * scale * ffn_ref[...]).astype(bf16)

    for d in ORDER + (0,):
        picked = jnp.dot(
            place_ref[d * group_rows : (d + 1) * group_rows, :],
            normed_ref[...],
            preferred_element_type=f32,
        )
        zsend[d] = picked.astype(bf16)
        if d:
            zcopy(d).start()

    def places(d):
        meta = meta_ref[0] if d == 0 else mrecv[d]
        row = lax.broadcasted_iota(jnp.int32, (slots, group_rows), 0).astype(jnp.float32)
        shift = (j * slot).astype(jnp.float32)
        out = []
        for k in range(2):
            at = meta[k : k + 1, :group_rows] - shift
            at = jnp.where(at < 0, at + slots, at)
            out.append(row == at)
        shares = [meta[2 + k : 3 + k, :group_rows] for k in range(2)]
        return out, shares

    def entry(d):
        if d:
            mcopy(d).wait_recv()
            zcopy(d).wait_recv()
        at, _ = places(d)
        chosen = jnp.where(at[0] | at[1], 1.0, 0.0).astype(jnp.bfloat16)
        rows = zsend[0] if d == 0 else zrecv[d]
        spread = jnp.dot(chosen, rows, preferred_element_type=jnp.float32).astype(jnp.bfloat16)
        xrecv[d, :slot] = spread[:slot]
        xsend[d, slot:] = spread[slot:]
        for o in range(1, peers):
            xcopy(d, o).start()

    def expert(d):
        for o in range(1, peers):
            xcopy(d, o).wait_recv()
        rows = xrecv[d]
        gate_out = jnp.dot(rows, gate_v[...], preferred_element_type=jnp.float32)
        up_out = jnp.dot(rows, up_v[...], preferred_element_type=jnp.float32)
        active = (gate_out / (1.0 + jnp.exp(-gate_out)) * up_out).astype(jnp.bfloat16)
        answer = jnp.dot(active, down_v[...], preferred_element_type=jnp.float32)
        answer = answer.astype(jnp.bfloat16)
        arecv[d, :slot] = answer[:slot]
        asend[d, slot:] = answer[slot:]
        for o in range(1, peers):
            acopy(d, o).start()

    def combine(d):
        for o in range(1, peers):
            acopy(d, o).wait_recv()
        at, shares = places(d)
        mix = jnp.where(at[0], shares[0], 0.0) + jnp.where(at[1], shares[1], 0.0)
        high = mix.astype(jnp.bfloat16)
        low = (mix - high.astype(jnp.float32)).astype(jnp.bfloat16)
        dims = (((0,), (0,)), ((), ()))
        answers = arecv[d]
        total = lax.dot_general(high, answers, dims, preferred_element_type=jnp.float32)
        total += lax.dot_general(low, answers, dims, preferred_element_type=jnp.float32)
        if d == 0:
            cret[0] = total.astype(jnp.bfloat16)
        else:
            csend[d] = total.astype(jnp.bfloat16)
            ccopy(d).start()

    a, b, c = ORDER
    entry(0)
    entry(a)
    for copy in weights:
        copy.wait()
    expert(0)
    entry(b)
    inner = (z >= 1) & (z < PLANES - 1)

    @pl.when(inner)
    def _():
        expert(a)
        combine(0)
        expert(b)
        combine(a)
        combine(b)
        entry(c)
        expert(c)
        combine(c)

    @pl.when(jnp.logical_not(inner))
    def _():
        expert(a)
        combine(0)
        entry(c)
        combine(a)
        expert(b)
        expert(c)
        combine(b)
        combine(c)

    for d in ORDER:
        ccopy(d).wait_recv()
    dims = (((0,), (0,)), ((), ()))
    gathered = cret[...].reshape(PLANES * group_rows, cret.shape[2])
    total = lax.dot_general(place_ref[...], gathered, dims, preferred_element_type=jnp.float32)
    out_ref[...] = (hidden_ref[...].astype(jnp.float32) + total).astype(jnp.bfloat16)

    halo().wait_send()
    for o in range(1, n_tp):
        tcopy(o).wait_send()
    for d in ORDER:
        mcopy(d).wait_send()
        zcopy(d).wait_send()
        ccopy(d).wait_send()
    for d in range(PLANES):
        for o in range(1, peers):
            xcopy(d, o).wait_send()
            acopy(d, o).wait_send()


def local(
    glu_value,
    glu_gate,
    conv_kernel,
    conv_bias,
    group_gain,
    group_shift,
    out_weight,
    residual,
    ffn_gain,
    expert_pick,
    pair_logits,
    group_prob,
    gate_weight,
    up_weight,
    down_weight,
):
    rows, width = residual.shape
    length, channels = glu_value.shape
    n_tp = lax.axis_size("tp")
    experts_all = lax.axis_size("sp") * n_tp
    cap = 4 * rows // experts_all
    peers = experts_all // PLANES
    group_rows = peers * cap // 2
    slot = max(cap, ROWS_MIN)
    slots = peers * slot
    lead = -(-(conv_kernel.shape[0] - 1) // 16) * 16
    bf16 = jnp.bfloat16
    f32 = jnp.float32
    vmem = pl.BlockSpec(memory_space=pltpu.VMEM)
    hbm = pl.BlockSpec(memory_space=pl.ANY)
    dma = pltpu.SemaphoreType.DMA
    return pl.pallas_call(
        functools.partial(layer_kernel, cap, slot),
        out_shape=jax.ShapeDtypeStruct((rows, width), bf16),
        in_specs=[vmem] * 11 + [hbm] * 4,
        out_specs=vmem,
        scratch_shapes=[
            pltpu.VMEM((lead + length, channels), f32),
            pltpu.VMEM((lead, channels), bf16),
            pltpu.VMEM((lead, channels), bf16),
            pltpu.VMEM((length, channels), bf16),
            pltpu.VMEM((n_tp, rows, channels), bf16),
            pltpu.VMEM((PLANES * group_rows, rows), bf16),
            pltpu.VMEM((PLANES, 8, 128), f32),
            pltpu.VMEM((rows, width), bf16),
            pltpu.VMEM((rows, width), bf16),
            pltpu.VMEM((rows, width), f32),
            pltpu.VMEM(out_weight.shape, bf16),
            pltpu.VMEM((PLANES, group_rows, width), bf16),
            pltpu.VMEM((PLANES, group_rows, width), bf16),
            pltpu.VMEM((PLANES, 8, 128), f32),
            pltpu.VMEM((PLANES, slots, width), bf16),
            pltpu.VMEM((PLANES, slots, width), bf16),
            pltpu.VMEM((PLANES, slots, width), bf16),
            pltpu.VMEM((PLANES, slots, width), bf16),
            pltpu.VMEM((PLANES, group_rows, width), bf16),
            pltpu.VMEM((PLANES, group_rows, width), bf16),
            pltpu.VMEM(gate_weight.shape[1:], bf16),
            pltpu.VMEM(up_weight.shape[1:], bf16),
            pltpu.VMEM(down_weight.shape[1:], bf16),
            dma((4,)),
            dma((1,)),
            dma((1,)),
            dma((n_tp,)),
            dma((n_tp,)),
            dma((PLANES,)),
            dma((PLANES,)),
            dma((PLANES,)),
            dma((PLANES,)),
            dma((PLANES, peers)),
            dma((PLANES, peers)),
            dma((PLANES, peers)),
            dma((PLANES, peers)),
            dma((PLANES,)),
            dma((PLANES,)),
        ],
        compiler_params=pltpu.CompilerParams(
            collective_id=0, has_side_effects=True, vmem_limit_bytes=62 * 1024 * 1024
        ),
    )(
        glu_value,
        glu_gate,
        conv_kernel,
        conv_bias[None, :],
        group_gain[None, :],
        group_shift[None, :],
        residual,
        ffn_gain[None, :],
        expert_pick,
        pair_logits,
        group_prob[None, :],
        out_weight,
        gate_weight,
        up_weight,
        down_weight,
    )


def solution(mesh):
    in_specs = (
        P("sp", "tp"),
        P("sp", "tp"),
        P(None, "tp"),
        P("tp"),
        P("tp"),
        P("tp"),
        P(),
        P(("sp", "tp"), None),
        P(),
        P(("sp", "tp"), None),
        P(("sp", "tp"), None),
        P(("sp", "tp")),
        P(("sp", "tp"), None, None),
        P(("sp", "tp"), None, None),
        P(("sp", "tp"), None, None),
    )
    out_specs = P(("sp", "tp"), None)
    return jax.shard_map(local, mesh=mesh, in_specs=in_specs, out_specs=out_specs, check_vma=False)
```

```python
import functools

import jax
import jax.numpy as jnp
from jax import lax
from jax.experimental import pallas as pl
from jax.experimental.pallas import tpu as pltpu
from jax.sharding import PartitionSpec as P

CONV_GROUPS = 8


EPS = 1e-06


PLANES = 4
MESH = pl.DeviceIdType.MESH
ORDER = (1, 3, 2)
ROWS_MIN = 16
HALVES = 2


def layer_kernel(
    cap,
    slot,
    value_ref,
    gate_ref,
    taps_ref,
    bias_ref,
    gain_ref,
    shift_ref,
    residual_ref,
    ffn_ref,
    pick_ref,
    logit_ref,
    prob_ref,
    out_hbm,
    gate_hbm,
    up_hbm,
    down_hbm,
    out_ref,
    glued,
    hsend,
    hrecv,
    mixed,
    mrest,
    place_ref,
    meta_ref,
    normed_ref,
    hidden_ref,
    proj,
    out_v,
    zsend,
    zrecv,
    mrecv,
    xsend,
    xrecv,
    asend,
    arecv,
    csend,
    cret,
    gate_v,
    up_v,
    down_v,
    wsem,
    hss,
    hrs,
    tss,
    trs,
    zss,
    zrs,
    mss,
    mrs,
    xss,
    xrs,
    ass,
    ars,
    css,
    crs,
):
    n_tp = lax.axis_size("tp")
    chips = lax.axis_size("sp") // PLANES
    peers = chips * n_tp
    sp = lax.axis_index("sp")
    tp = lax.axis_index("tp")
    n_sp = lax.axis_size("sp")
    z = sp // chips
    here = sp % chips
    tokens = residual_ref.shape[0]
    length, channels = value_ref.shape
    reach = taps_ref.shape[0] - 1
    lead = hsend.shape[0]
    j = here * n_tp + tp
    slots = peers * slot
    group_rows = zsend.shape[2]
    half = zsend.shape[3]

    def span(h):
        return slice(h * half, (h + 1) * half)

    def plane(d):
        if d == 1:
            return z + 1 - 2 * (z % 2)
        if d == 2:
            return z + 2 - 4 * (z // 2)
        return PLANES - 1 - z

    def mate(d):
        return (plane(d) * chips + here, tp)

    def peer(k):
        return (z * chips + k // n_tp, k % n_tp)

    def zcopy(d, h):
        return pltpu.make_async_remote_copy(
            src_ref=zsend.at[d, h], dst_ref=zrecv.at[d, h],
            send_sem=zss.at[d, h], recv_sem=zrs.at[d, h],
            device_id=mate(d), device_id_type=MESH,
        )

    def mcopy(d):
        return pltpu.make_async_remote_copy(
            src_ref=meta_ref.at[d], dst_ref=mrecv.at[d], send_sem=mss.at[d], recv_sem=mrs.at[d],
            device_id=mate(d), device_id_type=MESH,
        )

    def ccopy(d, h):
        return pltpu.make_async_remote_copy(
            src_ref=csend.at[d, h], dst_ref=cret.at[d, h],
            send_sem=css.at[d, h], recv_sem=crs.at[d, h],
            device_id=mate(d), device_id_type=MESH,
        )

    def xcopy(d, h, o):
        rows = pl.ds(o * slot, slot)
        return pltpu.make_async_remote_copy(
            src_ref=xsend.at[d, h, rows], dst_ref=xrecv.at[d, h, rows],
            send_sem=xss.at[d, h, o], recv_sem=xrs.at[d, h, o],
            device_id=peer((j + o) % peers), device_id_type=MESH,
        )

    def acopy(d, h, o):
        rows = pl.ds(o * slot, slot)
        return pltpu.make_async_remote_copy(
            src_ref=asend.at[d, h, rows], dst_ref=arecv.at[d, h, rows],
            send_sem=ass.at[d, h, o], recv_sem=ars.at[d, h, o],
            device_id=peer((j + peers - o) % peers), device_id_type=MESH,
        )

    def halo():
        return pltpu.make_async_remote_copy(
            src_ref=hsend, dst_ref=hrecv, send_sem=hss.at[0], recv_sem=hrs.at[0],
            device_id=((sp + 1) % n_sp, tp), device_id_type=MESH,
        )

    def tcopy(o):
        other = (tp + o) % n_tp
        rows = pl.ds(pl.multiple_of(other * tokens, tokens), tokens)
        return pltpu.make_async_remote_copy(
            src_ref=mixed.at[rows], dst_ref=mrest.at[o], send_sem=tss.at[o], recv_sem=trs.at[o],
            device_id=(sp, other), device_id_type=MESH,
        )

    out_copy = pltpu.make_async_copy(out_hbm, out_v, wsem.at[3])
    out_copy.start()
    weights = [
        pltpu.make_async_copy(gate_hbm.at[0], gate_v, wsem.at[0]),
        pltpu.make_async_copy(up_hbm.at[0], up_v, wsem.at[1]),
        pltpu.make_async_copy(down_hbm.at[0], down_v, wsem.at[2]),
    ]
    for copy in weights:
        copy.start()

    barrier = pltpu.get_barrier_semaphore()
    for d in ORDER:
        pl.semaphore_signal(barrier, inc=1, device_id=mate(d), device_id_type=MESH)
    for o in range(1, peers):
        pl.semaphore_signal(
            barrier, inc=1, device_id=peer((j + o) % peers), device_id_type=MESH
        )
    pl.semaphore_signal(
        barrier, inc=1, device_id=((sp + 1) % n_sp, tp), device_id_type=MESH
    )
    pl.semaphore_signal(
        barrier, inc=1, device_id=((sp + n_sp - 1) % n_sp, tp), device_id_type=MESH
    )

    f32 = jnp.float32
    bf16 = jnp.bfloat16
    block = 64
    for start in range(length - block, -1, -block):
        rows = slice(start, start + block)
        gated = value_ref[rows].astype(f32) / (1.0 + jnp.exp(-gate_ref[rows].astype(f32)))
        gated = gated.astype(bf16)
        glued[lead + start : lead + start + block] = gated.astype(f32)
        if start == length - block:
            hsend[...] = gated[block - lead :]
    pl.semaphore_wait(barrier, len(ORDER) + peers + 1)
    halo().start()

    lane = lax.broadcasted_iota(jnp.int32, (tokens, 128), 1)
    picks = pick_ref[...].astype(f32)
    logits = logit_ref[...]
    cols = [picks[:, 0:1], picks[:, 1:2], logits[:, 0:1], logits[:, 1:2]]
    wide = jnp.zeros((tokens, 128), f32)
    for k in range(4):
        wide = jnp.where(lane == k, cols[k], wide)
    tall = wide.T
    rows_of = [tall[k : k + 1, :] for k in range(4)]
    square = (tokens, tokens)
    earlier = lax.broadcasted_iota(jnp.int32, square, 0) < lax.broadcasted_iota(
        jnp.int32, square, 1
    )

    def group_of(pick):
        total = jnp.zeros(pick.shape, f32)
        for q in range(1, PLANES):
            total += jnp.where(pick >= (q * peers), 1.0, 0.0)
        return total

    def count(hit):
        return jnp.sum(jnp.where(hit & earlier, 1.0, 0.0), axis=0, keepdims=True)

    ranks = [count((cols[0] == r) | (cols[1] == r)) for r in rows_of[:2]]
    group_row = group_of(rows_of[0])
    spot = count(group_of(cols[0]) == group_row)
    away = group_row.astype(jnp.int32) ^ z
    at_row = away.astype(f32) * group_rows + spot
    row_id = lax.broadcasted_iota(jnp.int32, (PLANES * group_rows, tokens), 0).astype(f32)
    place_ref[...] = jnp.where(row_id == at_row, 1.0, 0.0).astype(bf16)
    gap = rows_of[2] - rows_of[3]
    shares = [prob_ref[...] / (1.0 + jnp.exp(-gap)), prob_ref[...] / (1.0 + jnp.exp(gap))]
    fields = [jnp.ones((1, tokens), f32)]
    for k in range(2):
        fields += [rows_of[k] - group_row * peers, ranks[k]]
    for share in shares:
        for _ in range(3):
            part = share.astype(bf16).astype(f32)
            fields.append(part)
            share = share - part
    field_id = lax.broadcasted_iota(jnp.int32, (16, tokens), 0)
    table = jnp.zeros((16, tokens), f32)
    for k, field in enumerate(fields):
        table = jnp.where(field_id == k, field, table)
    table = table.astype(bf16)
    meta_ref[...] = jnp.zeros(meta_ref.shape, f32)
    for d in range(PLANES):
        part = lax.dot_general(
            table,
            place_ref[d * group_rows : (d + 1) * group_rows, :],
            (((1,), (1,)), ((), ())),
            preferred_element_type=f32,
        )
        empty = (1.0 - part[0:1]) * 65536.0
        meta_ref[d, 0:1, :group_rows] = part[1:2] * slot + part[2:3] + empty
        meta_ref[d, 1:2, :group_rows] = part[3:4] * slot + part[4:5] + empty
        meta_ref[d, 2:3, :group_rows] = part[5:6] + part[6:7] + part[7:8]
        meta_ref[d, 3:4, :group_rows] = part[8:9] + part[9:10] + part[10:11]
    for d in ORDER:
        mcopy(d).start()

    wide_group = channels * n_tp // CONV_GROUPS
    taps = taps_ref[...].astype(f32)
    for start in range(length - block, -1, -block):
        if start == 0:
            halo().wait_recv()
            keep = jnp.where(sp > 0, 1.0, 0.0)
            glued[:lead] = hrecv[...].astype(f32) * keep
        for low_lane in range(0, channels, wide_group):
            part = slice(low_lane, low_lane + wide_group)
            total = jnp.zeros((block, wide_group), f32) + bias_ref[:, part]
            for offset in range(reach + 1):
                first = start + lead - reach + offset
                total += taps[offset : offset + 1, part] * glued[first : first + block, part]
            centre = jnp.mean(total, axis=-1, keepdims=True)
            total = total - centre
            variance = jnp.mean(total * total, axis=-1, keepdims=True)
            level = total * lax.rsqrt(variance + EPS)
            level = level * gain_ref[:, part] + shift_ref[:, part]
            mixed[start : start + block, part] = (level / (1.0 + jnp.exp(-level))).astype(bf16)
    for o in range(1, n_tp):
        tcopy(o).start()
    out_copy.wait()

    def weight_rows(which):
        return out_v[pl.ds(pl.multiple_of(which * channels, channels), channels), :]

    own = mixed[pl.ds(pl.multiple_of(tp * tokens, tokens), tokens), :]
    proj[...] = jnp.dot(own, weight_rows(tp), preferred_element_type=f32)
    for o in range(1, n_tp):
        tcopy(o).wait_recv()
        proj[...] += jnp.dot(
            mrest[o], weight_rows((tp + n_tp - o) % n_tp), preferred_element_type=f32
        )
    for start in range(0, tokens, 16):
        rows = slice(start, start + 16)
        hidden = (residual_ref[rows].astype(f32) + proj[rows]).astype(bf16)
        hidden_ref[rows] = hidden
        full = hidden.astype(f32)
        scale = lax.rsqrt(jnp.mean(full * full, axis=-1, keepdims=True) + EPS)
        normed_ref[rows] = (full * scale * ffn_ref[...]).astype(bf16)

    for d in ORDER + (0,):
        for h in range(HALVES):
            picked = jnp.dot(
                place_ref[d * group_rows : (d + 1) * group_rows, :],
                normed_ref[:, span(h)],
                preferred_element_type=f32,
            )
            zsend[d, h] = picked.astype(bf16)
            if d:
                zcopy(d, h).start()

    def places(d):
        meta = meta_ref[0] if d == 0 else mrecv[d]
        row = lax.broadcasted_iota(jnp.int32, (slots, group_rows), 0).astype(jnp.float32)
        shift = (j * slot).astype(jnp.float32)
        out = []
        for k in range(2):
            at = meta[k : k + 1, :group_rows] - shift
            at = jnp.where(at < 0, at + slots, at)
            out.append(row == at)
        shares = [meta[2 + k : 3 + k, :group_rows] for k in range(2)]
        return out, shares

    def entry(d):
        if d:
            mcopy(d).wait_recv()
        at, _ = places(d)
        chosen = jnp.where(at[0] | at[1], 1.0, 0.0).astype(jnp.bfloat16)
        for h in range(HALVES):
            if d:
                zcopy(d, h).wait_recv()
            rows = zsend[0, h] if d == 0 else zrecv[d, h]
            spread = jnp.dot(chosen, rows, preferred_element_type=jnp.float32)
            spread = spread.astype(jnp.bfloat16)
            xrecv[d, h, :slot] = spread[:slot]
            xsend[d, h, slot:] = spread[slot:]
            for o in range(1, peers):
                xcopy(d, h, o).start()

    def expert(d):
        gate_out = None
        for h in range(HALVES):
            for o in range(1, peers):
                xcopy(d, h, o).wait_recv()
            rows = xrecv[d, h]
            gate_part = jnp.dot(rows, gate_v[span(h), :], preferred_element_type=jnp.float32)
            up_part = jnp.dot(rows, up_v[span(h), :], preferred_element_type=jnp.float32)
            gate_out = gate_part if h == 0 else gate_out + gate_part
            up_out = up_part if h == 0 else up_out + up_part
        active = (gate_out / (1.0 + jnp.exp(-gate_out)) * up_out).astype(jnp.bfloat16)
        for h in range(HALVES):
            answer = jnp.dot(active, down_v[:, span(h)], preferred_element_type=jnp.float32)
            answer = answer.astype(jnp.bfloat16)
            arecv[d, h, :slot] = answer[:slot]
            asend[d, h, slot:] = answer[slot:]
            for o in range(1, peers):
                acopy(d, h, o).start()

    def combine(d):
        at, shares = places(d)
        mix = jnp.where(at[0], shares[0], 0.0) + jnp.where(at[1], shares[1], 0.0)
        high = mix.astype(jnp.bfloat16)
        low = (mix - high.astype(jnp.float32)).astype(jnp.bfloat16)
        dims = (((0,), (0,)), ((), ()))
        for h in range(HALVES):
            for o in range(1, peers):
                acopy(d, h, o).wait_recv()
            answers = arecv[d, h]
            total = lax.dot_general(high, answers, dims, preferred_element_type=jnp.float32)
            total += lax.dot_general(low, answers, dims, preferred_element_type=jnp.float32)
            if d == 0:
                cret[0, h] = total.astype(jnp.bfloat16)
            else:
                csend[d, h] = total.astype(jnp.bfloat16)
                ccopy(d, h).start()

    a, b, c = ORDER
    entry(0)
    entry(a)
    for copy in weights:
        copy.wait()
    expert(0)
    entry(b)
    inner = (z >= 1) & (z < PLANES - 1)

    @pl.when(inner)
    def _():
        expert(a)
        combine(0)
        expert(b)
        combine(a)
        combine(b)
        entry(c)
        expert(c)
        combine(c)

    @pl.when(jnp.logical_not(inner))
    def _():
        expert(a)
        combine(0)
        entry(c)
        combine(a)
        expert(b)
        expert(c)
        combine(b)
        combine(c)

    dims = (((0,), (0,)), ((), ()))
    for h in range(HALVES):
        total = hidden_ref[:, span(h)].astype(jnp.float32)
        for d in (0,) + ORDER:
            if d:
                ccopy(d, h).wait_recv()
            total += lax.dot_general(
                place_ref[d * group_rows : (d + 1) * group_rows, :],
                cret[d, h],
                dims,
                preferred_element_type=jnp.float32,
            )
        out_ref[:, span(h)] = total.astype(jnp.bfloat16)

    halo().wait_send()
    for o in range(1, n_tp):
        tcopy(o).wait_send()
    for d in ORDER:
        mcopy(d).wait_send()
        for h in range(HALVES):
            zcopy(d, h).wait_send()
            ccopy(d, h).wait_send()
    for d in range(PLANES):
        for h in range(HALVES):
            for o in range(1, peers):
                xcopy(d, h, o).wait_send()
                acopy(d, h, o).wait_send()


def local(
    glu_value,
    glu_gate,
    conv_kernel,
    conv_bias,
    group_gain,
    group_shift,
    out_weight,
    residual,
    ffn_gain,
    expert_pick,
    pair_logits,
    group_prob,
    gate_weight,
    up_weight,
    down_weight,
):
    rows, width = residual.shape
    length, channels = glu_value.shape
    n_tp = lax.axis_size("tp")
    experts_all = lax.axis_size("sp") * n_tp
    cap = 4 * rows // experts_all
    peers = experts_all // PLANES
    group_rows = peers * cap // 2
    slot = max(cap, ROWS_MIN)
    slots = peers * slot
    lead = -(-(conv_kernel.shape[0] - 1) // 16) * 16
    bf16 = jnp.bfloat16
    f32 = jnp.float32
    vmem = pl.BlockSpec(memory_space=pltpu.VMEM)
    hbm = pl.BlockSpec(memory_space=pl.ANY)
    dma = pltpu.SemaphoreType.DMA
    return pl.pallas_call(
        functools.partial(layer_kernel, cap, slot),
        out_shape=jax.ShapeDtypeStruct((rows, width), bf16),
        in_specs=[vmem] * 11 + [hbm] * 4,
        out_specs=vmem,
        scratch_shapes=[
            pltpu.VMEM((lead + length, channels), f32),
            pltpu.VMEM((lead, channels), bf16),
            pltpu.VMEM((lead, channels), bf16),
            pltpu.VMEM((length, channels), bf16),
            pltpu.VMEM((n_tp, rows, channels), bf16),
            pltpu.VMEM((PLANES * group_rows, rows), bf16),
            pltpu.VMEM((PLANES, 8, 128), f32),
            pltpu.VMEM((rows, width), bf16),
            pltpu.VMEM((rows, width), bf16),
            pltpu.VMEM((rows, width), f32),
            pltpu.VMEM(out_weight.shape, bf16),
            pltpu.VMEM((PLANES, HALVES, group_rows, width // HALVES), bf16),
            pltpu.VMEM((PLANES, HALVES, group_rows, width // HALVES), bf16),
            pltpu.VMEM((PLANES, 8, 128), f32),
            pltpu.VMEM((PLANES, HALVES, slots, width // HALVES), bf16),
            pltpu.VMEM((PLANES, HALVES, slots, width // HALVES), bf16),
            pltpu.VMEM((PLANES, HALVES, slots, width // HALVES), bf16),
            pltpu.VMEM((PLANES, HALVES, slots, width // HALVES), bf16),
            pltpu.VMEM((PLANES, HALVES, group_rows, width // HALVES), bf16),
            pltpu.VMEM((PLANES, HALVES, group_rows, width // HALVES), bf16),
            pltpu.VMEM(gate_weight.shape[1:], bf16),
            pltpu.VMEM(up_weight.shape[1:], bf16),
            pltpu.VMEM(down_weight.shape[1:], bf16),
            dma((4,)),
            dma((1,)),
            dma((1,)),
            dma((n_tp,)),
            dma((n_tp,)),
            dma((PLANES, HALVES)),
            dma((PLANES, HALVES)),
            dma((PLANES,)),
            dma((PLANES,)),
            dma((PLANES, HALVES, peers)),
            dma((PLANES, HALVES, peers)),
            dma((PLANES, HALVES, peers)),
            dma((PLANES, HALVES, peers)),
            dma((PLANES, HALVES)),
            dma((PLANES, HALVES)),
        ],
        compiler_params=pltpu.CompilerParams(
            collective_id=0, has_side_effects=True, vmem_limit_bytes=62 * 1024 * 1024
        ),
    )(
        glu_value,
        glu_gate,
        conv_kernel,
        conv_bias[None, :],
        group_gain[None, :],
        group_shift[None, :],
        residual,
        ffn_gain[None, :],
        expert_pick,
        pair_logits,
        group_prob[None, :],
        out_weight,
        gate_weight,
        up_weight,
        down_weight,
    )


def solution(mesh):
    in_specs = (
        P("sp", "tp"),
        P("sp", "tp"),
        P(None, "tp"),
        P("tp"),
        P("tp"),
        P("tp"),
        P(),
        P(("sp", "tp"), None),
        P(),
        P(("sp", "tp"), None),
        P(("sp", "tp"), None),
        P(("sp", "tp")),
        P(("sp", "tp"), None, None),
        P(("sp", "tp"), None, None),
        P(("sp", "tp"), None, None),
    )
    out_specs = P(("sp", "tp"), None)
    return jax.shard_map(local, mesh=mesh, in_specs=in_specs, out_specs=out_specs, check_vma=False)
```
